32 devices in a mesh: sp: 16 (over z, y, x), tp: 2 (over core).
Axes of the slice: x: 2, y: 2, z: 4, core: 2. Of those that a mesh axis runs over, the one named last changes fastest.
Arguments:
- queries: bfloat16 [3072, 1024], P('sp', 'tp'), may hold values from -6 to 6
- keys: bfloat16 [3072, 512], P('sp', 'tp'), may hold values from -6 to 6
- values: bfloat16 [3072, 512], P('sp', 'tp'), may hold values from -6 to 6
- query_gain: float32 [16, 64], P('tp'), may hold values from 1.4 to 7.5
- key_gain: float32 [8, 64], P('tp'), may hold values from 1.4 to 7.5
- out_weight: bfloat16 [1024, 2048], P('tp'), may hold values from -0.375 to 0.375
- residual: bfloat16 [3072, 2048], P('sp'), may hold values from -170 to 170
- norm_gain: float32 [2048], replicated, may hold values from 0.1 to 1.9
- gate_weight: bfloat16 [2048, 5632], P('sp', 'tp'), may hold values from -0.125 to 0.125
- up_weight: bfloat16 [2048, 5632], P('sp', 'tp'), may hold values from -0.125 to 0.125
- down_weight: bfloat16 [5632, 2048], P('tp', 'sp'), may hold values from -0.15625 to 0.15625
Outputs:
- mixed: bfloat16 [3072, 2048], P('sp')
The draws below stay inside these ranges and needn't reach their ends.
All inputs are finite; a program needn't handle non-finite values.
Results may differ from the reference program's by a relative error of at most 0.017.
Values may be sent and summed in bfloat16 or wider, within the bound.
A program may use at most 128 MiB of HBM per device.

```python
import math
import jax
import jax.numpy as jnp
from jax import lax

D = 2048
FF = 5632
HEADS = 16
KV_HEADS = 8
HEAD_SIZE = 64
GRID_W = 64
SEQ = 3072
N_TP = 2


def drawn_keys(key):
    base_keys = jnp.clip(jax.random.normal(jax.random.fold_in(key, 11), (SEQ, KV_HEADS * HEAD_SIZE), jnp.float32), -6.0, 6.0)
    return base_keys


def draw_keys(key, part):
    base_keys = drawn_keys(key)
    return base_keys.astype(jnp.bfloat16)


def draw_queries(key, part):
    fresh = jnp.clip(jax.random.normal(jax.random.fold_in(key, 12), (SEQ, HEADS * HEAD_SIZE), jnp.float32), -6.0, 6.0)
    return fresh.astype(jnp.bfloat16)


def draw_values(key, part):
    column_sign = jnp.where(jax.random.uniform(jax.random.fold_in(key, 51), (1, KV_HEADS * HEAD_SIZE), jnp.float32) < 0.5, -1.0, 1.0)
    noise = jax.random.normal(jax.random.fold_in(key, 52), (SEQ, KV_HEADS * HEAD_SIZE), jnp.float32)
    return jnp.clip(2.0 * column_sign + noise, -6.0, 6.0).astype(jnp.bfloat16)


def gain_levels(key, count, salt):
    lower, upper = (1.7, 2.0)
    level = jnp.exp(jax.random.uniform(jax.random.fold_in(key, salt), (count, 1), jnp.float32, jnp.log(lower), jnp.log(upper)))
    rough = jax.random.uniform(jax.random.fold_in(key, salt + 1), (count, HEAD_SIZE), jnp.float32, 0.85, 1.15)
    return level * rough


def draw_query_gain(key, part):
    return gain_levels(key, HEADS, 31)


def draw_key_gain(key, part):
    return gain_levels(key, KV_HEADS, 41)


def draw_residual(key, part):
    base = jnp.clip(jax.random.normal(jax.random.fold_in(key, 21), (SEQ, D), jnp.float32), -6.0, 6.0)
    row_scale = jnp.exp(jax.random.uniform(jax.random.fold_in(key, 22), (SEQ, 1), jnp.float32, jnp.log(0.3), jnp.log(3.0)))
    col_scale = jnp.exp(jax.random.uniform(jax.random.fold_in(key, 23), (1, D), jnp.float32, jnp.log(0.3), jnp.log(3.0)))
    result = base * row_scale * col_scale
    return result.astype(jnp.bfloat16)


def steps_of(stream_key, shape, shards, low, largest):
    level = 1.0
    for dim, parts in shards:
        steps = jax.random.uniform(jax.random.fold_in(jax.random.fold_in(stream_key, 6), dim), (parts,), jnp.float32, low / len(shards), largest / len(shards))
        level = level * jnp.repeat(jnp.exp(steps), shape[dim] // parts).reshape((-1,) + (1,) * (len(shape) - 1 - dim))
    return level


def normal_values(key, extent, scale, most, pieces=(), held_as=jnp.bfloat16):
    values = scale * jax.random.normal(key, extent, jnp.float32)
    if pieces:
        values = values * steps_of(key, extent, pieces, -0.22, 0.18)
    return jnp.clip(values, -most, most).astype(held_as)


def setup_inputs(seed: int = 0) -> dict:
    key_list = jax.random.split(jax.random.key(seed), 12)
    queries = draw_queries(jax.random.fold_in(key_list[11], 71), 0)
    keys = draw_keys(jax.random.fold_in(key_list[11], 71), 0)
    values = draw_values(jax.random.fold_in(key_list[11], 71), 0)
    query_gain = draw_query_gain(jax.random.fold_in(key_list[11], 71), 0)
    key_gain = draw_key_gain(jax.random.fold_in(key_list[11], 71), 0)
    out_weight = normal_values(key_list[5], (HEADS * HEAD_SIZE, D), (HEADS * HEAD_SIZE // 4) ** -0.5, 0.375, ((0, 2),))
    residual = draw_residual(jax.random.fold_in(key_list[11], 71), 0)
    norm_gain = jnp.clip(1.0 + 0.18 * jax.random.normal(key_list[7], (D,), jnp.float32), 0.1, 1.9)
    gate_weight = normal_values(key_list[8], (D, FF), D ** -0.5, 0.125, ((0, 16), (1, 2)))
    up_weight = normal_values(key_list[9], (D, FF), D ** -0.5, 0.125, ((0, 16), (1, 2)))
    down_weight = normal_values(key_list[10], (FF, D), (FF // 4) ** -0.5, 0.15625, ((0, 2), (1, 16)))
    return dict(queries=queries, keys=keys, values=values, query_gain=query_gain, key_gain=key_gain, out_weight=out_weight, residual=residual, norm_gain=norm_gain, gate_weight=gate_weight, up_weight=up_weight, down_weight=down_weight)


epsilon = 1e-06
rope_base = 10000.0

def rotate_pairs(entries, places):
    half = entries.shape[-1] // 2
    frequency = rope_base ** (-jnp.arange(half, dtype=jnp.float32) / half)
    angle = places.astype(jnp.float32)[:, None, None] * frequency[None, None, :]
    cosine = jnp.cos(angle)
    sine = jnp.sin(angle)
    first = entries[..., :half]
    second = entries[..., half:]
    return jnp.concatenate([first * cosine - second * sine, first * sine + second * cosine], axis=-1)

def grid_rotate(entries, grid_rows, grid_cols):
    half = entries.shape[-1] // 2
    return jnp.concatenate([rotate_pairs(entries[..., :half], grid_rows), rotate_pairs(entries[..., half:], grid_cols)], axis=-1)

def head_norm(entries, gains):
    factor = lax.rsqrt(lax.optimization_barrier(jnp.mean(entries * entries, axis=-1, keepdims=True)) + epsilon)
    return entries * factor * gains[None]

def reference(queries, keys, values, query_gain, key_gain, out_weight, residual, norm_gain, gate_weight, up_weight, down_weight):
    length = queries.shape[0]
    heads = query_gain.shape[0]
    key_heads = key_gain.shape[0]
    head_size = query_gain.shape[1]
    group = heads // key_heads
    places = jnp.arange(length, dtype=jnp.int32)
    grid_rows = places // GRID_W
    grid_cols = places % GRID_W
    query_turned = grid_rotate(head_norm(queries.astype(jnp.float32).reshape(length, heads, head_size), query_gain), grid_rows, grid_cols).astype(jnp.bfloat16)
    key_turned = grid_rotate(head_norm(keys.astype(jnp.float32).reshape(length, key_heads, head_size), key_gain), grid_rows, grid_cols).astype(jnp.bfloat16)
    key_wide = key_turned.astype(jnp.float32)
    value_wide = values.reshape(length, key_heads, head_size).astype(jnp.float32)
    scale = head_size ** (-0.5)
    block = math.gcd(length, 128)
    query_blocks = query_turned.reshape(length // block, block, key_heads, group, head_size)

    def attend(query_block):
        scores = jnp.einsum('qgrd,kgd->qgrk', query_block.astype(jnp.float32), key_wide) * scale
        top = lax.optimization_barrier(jnp.max(scores, axis=-1, keepdims=True))
        weights = jnp.exp(scores - top)
        total = lax.optimization_barrier(jnp.sum(weights, axis=-1))
        rounded = lax.optimization_barrier(weights.astype(jnp.bfloat16)).astype(jnp.float32)
        summed = jnp.einsum('qgrk,kgd->qgrd', rounded, value_wide)
        return summed / total[..., None]
    attended = lax.map(attend, query_blocks).reshape(length, heads * head_size).astype(jnp.bfloat16)
    head_cols = heads * head_size // N_TP
    branch = jnp.zeros((length, out_weight.shape[1]), jnp.float32)
    for index in range(N_TP):
        partial_sum = jnp.dot(attended[:, index * head_cols:(index + 1) * head_cols], out_weight[index * head_cols:(index + 1) * head_cols], preferred_element_type=jnp.float32)
        branch = branch + lax.optimization_barrier(partial_sum.astype(jnp.bfloat16)).astype(jnp.float32)
    mid = (residual.astype(jnp.float32) + branch).astype(jnp.bfloat16)
    mid_wide = mid.astype(jnp.float32)
    normed = (mid_wide * lax.rsqrt(lax.optimization_barrier(jnp.mean(mid_wide * mid_wide, axis=-1, keepdims=True)) + epsilon) * norm_gain).astype(jnp.bfloat16)
    gate = jnp.dot(normed, gate_weight, preferred_element_type=jnp.float32)
    up_value = jnp.dot(normed, up_weight, preferred_element_type=jnp.float32)
    hidden = (jax.nn.silu(gate) * up_value).astype(jnp.bfloat16)
    unit_cols = gate_weight.shape[1] // N_TP
    ffn = jnp.zeros((length, down_weight.shape[1]), jnp.float32)
    for index in range(N_TP):
        partial_sum = jnp.dot(hidden[:, index * unit_cols:(index + 1) * unit_cols], down_weight[index * unit_cols:(index + 1) * unit_cols], preferred_element_type=jnp.float32)
        ffn = ffn + lax.optimization_barrier(partial_sum.astype(jnp.bfloat16)).astype(jnp.float32)
    return (mid.astype(jnp.float32) + ffn).astype(jnp.bfloat16)
```

```python
import jax
import jax.numpy as jnp
from jax import lax
from jax.sharding import PartitionSpec as P

GRID_W = 64


epsilon = 1e-06
rope_base = 10000.0
block_keys = 2048


def rotate_pairs(entries, places):
    half = entries.shape[-1] // 2
    frequency = rope_base ** (-jnp.arange(half, dtype=jnp.float32) / half)
    angle = places.astype(jnp.float32)[:, None, None] * frequency[None, None, :]
    cosine = jnp.cos(angle)
    sine = jnp.sin(angle)
    first = entries[..., :half]
    second = entries[..., half:]
    return jnp.concatenate(
        [first * cosine - second * sine, first * sine + second * cosine], axis=-1
    )


def grid_rotate(entries, grid_rows, grid_cols):
    half = entries.shape[-1] // 2
    return jnp.concatenate(
        [
            rotate_pairs(entries[..., :half], grid_rows),
            rotate_pairs(entries[..., half:], grid_cols),
        ],
        axis=-1,
    )


def head_norm(entries, gains):
    factor = lax.rsqrt(jnp.mean(entries * entries, axis=-1, keepdims=True) + epsilon)
    return entries * factor * gains[None]


def row_norm(mid, norm_gain):
    wide = mid.astype(jnp.float32)
    return (
        wide * lax.rsqrt(jnp.mean(wide * wide, axis=-1, keepdims=True) + epsilon) * norm_gain
    ).astype(jnp.bfloat16)


def block_span(length):
    if length <= block_keys:
        return length
    span = block_keys
    while length % span != 0:
        span = span - 1
    return span


def sub_groups(size, units):
    ways = 4
    while size % ways != 0 or units % ways != 0:
        ways = ways // 2
    blocks = size // ways
    lines = [[way * blocks + block for way in range(ways)] for block in range(blocks)]
    planes = [[way * blocks + block for block in range(blocks)] for way in range(ways)]
    return ways, lines, planes


def swap_blocks(rows, outer, inner):
    count, width = rows.shape
    cut = rows.reshape(count, outer, inner, width // (outer * inner))
    return cut.transpose(0, 2, 1, 3).reshape(count, width)


def line_columns(weight, ways, lines):
    rows, units = weight.shape
    pieces = weight.reshape(rows, ways, units // ways).transpose(1, 0, 2)
    line = lax.all_to_all(pieces, "sp", 0, 0, axis_index_groups=lines)
    return line.reshape(ways * rows, units // ways)


def line_rows(weight, ways, lines):
    units, columns = weight.shape
    pieces = weight.reshape(ways, units // ways, columns)
    return lax.all_to_all(pieces, "sp", 0, 0, axis_index_groups=lines)


def plane_gather(line, planes):
    return lax.all_gather(line, "sp", axis=0, tiled=True, axis_index_groups=planes)


def gather_pair(keys, values, lines, planes):
    width = keys.shape[1]
    both = jnp.concatenate([keys, values], axis=1)
    line = lax.all_gather(both, "sp", axis=0, tiled=True, axis_index_groups=lines)
    every = lax.all_gather(line, "sp", axis=0, tiled=True, axis_index_groups=planes)
    return every[:, :width], every[:, width:]


def body(
    queries,
    keys,
    values,
    query_gain,
    key_gain,
    out_weight,
    residual,
    norm_gain,
    gate_weight,
    up_weight,
    down_weight,
):
    own = queries.shape[0]
    heads = query_gain.shape[0]
    key_heads = key_gain.shape[0]
    head_size = query_gain.shape[1]
    group = heads // key_heads
    ways, lines, planes = sub_groups(lax.axis_size("sp"), gate_weight.shape[1])
    gate_line = line_columns(gate_weight, ways, lines)
    up_line = line_columns(up_weight, ways, lines)
    down_line = line_rows(down_weight, ways, lines)
    keys, queries, gate_line, up_line, down_line = lax.optimization_barrier(
        (keys, queries, gate_line, up_line, down_line)
    )
    places = lax.axis_index("sp") * own + jnp.arange(own, dtype=jnp.int32)
    grid_rows = places // GRID_W
    grid_cols = places % GRID_W
    query_turned = grid_rotate(
        head_norm(queries.astype(jnp.float32).reshape(own, heads, head_size), query_gain),
        grid_rows,
        grid_cols,
    ).astype(jnp.bfloat16)
    query_groups = query_turned.reshape(own, key_heads, group, head_size)
    key_turned = (
        grid_rotate(
            head_norm(keys.astype(jnp.float32).reshape(own, key_heads, head_size), key_gain),
            grid_rows,
            grid_cols,
        )
        .astype(jnp.bfloat16)
        .reshape(own, key_heads * head_size)
    )
    scale = head_size ** (-0.5)

    def absorb(carry, key_block, value_block):
        top, total, summed = carry
        key_block = key_block.reshape(-1, key_heads, head_size)
        value_block = value_block.reshape(-1, key_heads, head_size)
        score = (
            jnp.einsum(
                "qgrd,kgd->qgrk", query_groups, key_block, preferred_element_type=jnp.float32
            )
            * scale
        )
        new_top = jnp.maximum(top, jnp.max(score, axis=-1))
        weight = jnp.exp(score - new_top[..., None])
        shrink = jnp.exp(top - new_top)
        total = total * shrink + jnp.sum(weight, axis=-1)
        summed = summed * shrink[..., None] + jnp.einsum(
            "qgrk,kgd->qgrd",
            weight.astype(jnp.bfloat16),
            value_block,
            preferred_element_type=jnp.float32,
        )
        return (new_top, total, summed)

    def fold_keys(carry, pieces):
        length = pieces[0].shape[0]
        span = block_span(length)
        if span == length:
            return absorb(carry, pieces[0], pieces[1])
        width = pieces[0].shape[1]
        key_blocks = pieces[0].reshape(length // span, span, width)
        value_blocks = pieces[1].reshape(length // span, span, width)

        def scan_step(inner, blocks):
            return (absorb(inner, blocks[0], blocks[1]), None)

        result, unused = lax.scan(scan_step, carry, (key_blocks, value_blocks))
        return result

    start_state = (
        jnp.full((own, key_heads, group), -jnp.inf, jnp.float32),
        jnp.zeros((own, key_heads, group), jnp.float32),
        jnp.zeros((own, key_heads, group, head_size), jnp.float32),
    )
    all_keys, all_values = gather_pair(key_turned, values, lines, planes)
    all_keys, all_values, gate_line, up_line, down_line = lax.optimization_barrier(
        (all_keys, all_values, gate_line, up_line, down_line)
    )
    gate_full = plane_gather(gate_line, planes)
    up_full = plane_gather(up_line, planes)
    down_full = plane_gather(down_line, planes)
    down_full = down_full.transpose(1, 0, 2).reshape(down_full.shape[1], -1)
    top, total, summed = fold_keys(start_state, (all_keys, all_values))
    attended = (summed / total[..., None]).reshape(own, heads * head_size).astype(jnp.bfloat16)
    attended, gate_full, up_full = lax.optimization_barrier((attended, gate_full, up_full))
    part_rows = own // lax.axis_size("tp")
    branch = lax.psum_scatter(
        jnp.dot(
            lax.slice_in_dim(attended, 0, lax.axis_size("tp") * part_rows, axis=0),
            out_weight,
            preferred_element_type=jnp.float32,
        ).astype(jnp.bfloat16),
        "tp",
        scatter_dimension=0,
        tiled=True,
    ).astype(jnp.float32)
    own_rows = lax.dynamic_slice_in_dim(residual, lax.axis_index("tp") * part_rows, part_rows, 0)
    mid = (own_rows.astype(jnp.float32) + branch).astype(jnp.bfloat16)
    blocks = lax.axis_size("sp") // ways
    normed = row_norm(mid, norm_gain)
    normed = swap_blocks(normed, ways, blocks)
    normed_line = lax.all_gather(normed, "sp", axis=0, tiled=True, axis_index_groups=lines)
    normed_all = lax.all_gather(normed_line, "tp", axis=0, tiled=True)
    gate = jnp.dot(normed_all, gate_full, preferred_element_type=jnp.float32)
    up_value = jnp.dot(normed_all, up_full, preferred_element_type=jnp.float32)
    hidden = (jax.nn.silu(gate) * up_value).astype(jnp.bfloat16)
    terms = jnp.dot(hidden, down_full, preferred_element_type=jnp.float32)
    line_terms = lax.psum_scatter(
        terms.astype(jnp.bfloat16), "tp", scatter_dimension=0, tiled=True
    )
    ffn = lax.psum_scatter(
        line_terms, "sp", scatter_dimension=0, tiled=True, axis_index_groups=lines
    ).astype(jnp.float32)
    ffn = swap_blocks(ffn, blocks, ways)
    finished = (mid.astype(jnp.float32) + ffn).astype(jnp.bfloat16)
    return lax.all_gather(finished, "tp", axis=0, tiled=True)


def solution(mesh):
    in_specs = (
        P("sp", "tp"),
        P("sp", "tp"),
        P("sp", "tp"),
        P("tp", None),
        P("tp", None),
        P("tp", None),
        P("sp", None),
        P(),
        P("sp", "tp"),
        P("sp", "tp"),
        P("tp", "sp"),
    )
    out_specs = P("sp", None)
    return jax.shard_map(body, mesh=mesh, in_specs=in_specs, out_specs=out_specs, check_vma=False)
```

```python
import jax
import jax.numpy as jnp
from jax import lax
from jax.sharding import PartitionSpec as P

GRID_W = 64


epsilon = 1e-06
rope_base = 10000.0
block_keys = 2048


def rotate_pairs(entries, places):
    half = entries.shape[-1] // 2
    frequency = rope_base ** (-jnp.arange(half, dtype=jnp.float32) / half)
    angle = places.astype(jnp.float32)[:, None, None] * frequency[None, None, :]
    cosine = jnp.cos(angle)
    sine = jnp.sin(angle)
    first = entries[..., :half]
    second = entries[..., half:]
    return jnp.concatenate(
        [first * cosine - second * sine, first * sine + second * cosine], axis=-1
    )


def grid_rotate(entries, grid_rows, grid_cols):
    half = entries.shape[-1] // 2
    return jnp.concatenate(
        [
            rotate_pairs(entries[..., :half], grid_rows),
            rotate_pairs(entries[..., half:], grid_cols),
        ],
        axis=-1,
    )


def head_norm(entries, gains):
    factor = lax.rsqrt(jnp.mean(entries * entries, axis=-1, keepdims=True) + epsilon)
    return entries * factor * gains[None]


def row_norm(mid, norm_gain):
    wide = mid.astype(jnp.float32)
    return (
        wide * lax.rsqrt(jnp.mean(wide * wide, axis=-1, keepdims=True) + epsilon) * norm_gain
    ).astype(jnp.bfloat16)


def block_span(length):
    if length <= block_keys:
        return length
    span = block_keys
    while length % span != 0:
        span = span - 1
    return span


def sub_groups(size, units):
    ways = 4
    while size % ways != 0 or units % ways != 0:
        ways = ways // 2
    blocks = size // ways
    lines = [[way * blocks + block for way in range(ways)] for block in range(blocks)]
    planes = [[way * blocks + block for block in range(blocks)] for way in range(ways)]
    return ways, lines, planes


def swap_blocks(rows, outer, inner):
    count, width = rows.shape
    cut = rows.reshape(count, outer, inner, width // (outer * inner))
    return cut.transpose(0, 2, 1, 3).reshape(count, width)


def line_columns(weight, ways, lines):
    rows, units = weight.shape
    pieces = weight.reshape(rows, ways, units // ways).transpose(1, 0, 2)
    line = lax.all_to_all(pieces, "sp", 0, 0, axis_index_groups=lines)
    return line.reshape(ways * rows, units // ways)


def line_rows(weight, ways, lines):
    units, columns = weight.shape
    pieces = weight.reshape(ways, units // ways, columns)
    return lax.all_to_all(pieces, "sp", 0, 0, axis_index_groups=lines)


def plane_gather(line, planes):
    return lax.all_gather(line, "sp", axis=0, tiled=True, axis_index_groups=planes)


def gather_pair(keys, values, lines):
    both = jnp.concatenate([keys, values], axis=1)
    return lax.all_gather(both, "sp", axis=0, tiled=True, axis_index_groups=lines)


def body(
    queries,
    keys,
    values,
    query_gain,
    key_gain,
    out_weight,
    residual,
    norm_gain,
    gate_weight,
    up_weight,
    down_weight,
):
    own = queries.shape[0]
    heads = query_gain.shape[0]
    key_heads = key_gain.shape[0]
    head_size = query_gain.shape[1]
    group = heads // key_heads
    ways, lines, planes = sub_groups(lax.axis_size("sp"), gate_weight.shape[1])
    places = lax.axis_index("sp") * own + jnp.arange(own, dtype=jnp.int32)
    grid_rows = places // GRID_W
    grid_cols = places % GRID_W
    query_turned = grid_rotate(
        head_norm(queries.astype(jnp.float32).reshape(own, heads, head_size), query_gain),
        grid_rows,
        grid_cols,
    ).astype(jnp.bfloat16)
    query_groups = query_turned.reshape(own, key_heads, group, head_size)
    key_turned = (
        grid_rotate(
            head_norm(keys.astype(jnp.float32).reshape(own, key_heads, head_size), key_gain),
            grid_rows,
            grid_cols,
        )
        .astype(jnp.bfloat16)
        .reshape(own, key_heads * head_size)
    )
    scale = head_size ** (-0.5)

    def absorb(carry, key_block, value_block):
        top, total, summed = carry
        key_block = key_block.reshape(-1, key_heads, head_size)
        value_block = value_block.reshape(-1, key_heads, head_size)
        score = (
            jnp.einsum(
                "qgrd,kgd->qgrk", query_groups, key_block, preferred_element_type=jnp.float32
            )
            * scale
        )
        new_top = jnp.maximum(top, jnp.max(score, axis=-1))
        weight = jnp.exp(score - new_top[..., None])
        shrink = jnp.exp(top - new_top)
        total = total * shrink + jnp.sum(weight, axis=-1)
        summed = summed * shrink[..., None] + jnp.einsum(
            "qgrk,kgd->qgrd",
            weight.astype(jnp.bfloat16),
            value_block,
            preferred_element_type=jnp.float32,
        )
        return (new_top, total, summed)

    def fold_keys(carry, pieces):
        length = pieces[0].shape[0]
        span = block_span(length)
        if span == length:
            return absorb(carry, pieces[0], pieces[1])
        width = pieces[0].shape[1]
        key_blocks = pieces[0].reshape(length // span, span, width)
        value_blocks = pieces[1].reshape(length // span, span, width)

        def scan_step(inner, blocks):
            return (absorb(inner, blocks[0], blocks[1]), None)

        result, unused = lax.scan(scan_step, carry, (key_blocks, value_blocks))
        return result

    start_state = (
        jnp.full((own, key_heads, group), -jnp.inf, jnp.float32),
        jnp.zeros((own, key_heads, group), jnp.float32),
        jnp.zeros((own, key_heads, group, head_size), jnp.float32),
    )
    pair_line = gather_pair(key_turned, values, lines)
    pair_line, gate_weight, up_weight, down_weight = lax.optimization_barrier(
        (pair_line, gate_weight, up_weight, down_weight)
    )
    pair = plane_gather(pair_line, planes)
    all_keys, all_values = pair[:, : keys.shape[1]], pair[:, keys.shape[1] :]
    gate_line = line_columns(gate_weight, ways, lines)
    up_line = line_columns(up_weight, ways, lines)
    down_line = line_rows(down_weight, ways, lines)
    all_keys, all_values, gate_line, up_line, down_line = lax.optimization_barrier(
        (all_keys, all_values, gate_line, up_line, down_line)
    )
    gate_full = plane_gather(gate_line, planes)
    up_full = plane_gather(up_line, planes)
    down_full = plane_gather(down_line, planes)
    down_full = down_full.transpose(1, 0, 2).reshape(down_full.shape[1], -1)
    top, total, summed = fold_keys(start_state, (all_keys, all_values))
    attended = (summed / total[..., None]).reshape(own, heads * head_size).astype(jnp.bfloat16)
    attended, gate_full, up_full = lax.optimization_barrier((attended, gate_full, up_full))
    part_rows = own // lax.axis_size("tp")
    branch = lax.psum_scatter(
        jnp.dot(
            lax.slice_in_dim(attended, 0, lax.axis_size("tp") * part_rows, axis=0),
            out_weight,
            preferred_element_type=jnp.float32,
        ).astype(jnp.bfloat16),
        "tp",
        scatter_dimension=0,
        tiled=True,
    ).astype(jnp.float32)
    own_rows = lax.dynamic_slice_in_dim(residual, lax.axis_index("tp") * part_rows, part_rows, 0)
    mid = (own_rows.astype(jnp.float32) + branch).astype(jnp.bfloat16)
    blocks = lax.axis_size("sp") // ways
    normed = row_norm(mid, norm_gain)
    normed = swap_blocks(normed, ways, blocks)
    normed_line = lax.all_gather(normed, "sp", axis=0, tiled=True, axis_index_groups=lines)
    normed_all = lax.all_gather(normed_line, "tp", axis=0, tiled=True)
    gate = jnp.dot(normed_all, gate_full, preferred_element_type=jnp.float32)
    up_value = jnp.dot(normed_all, up_full, preferred_element_type=jnp.float32)
    hidden = (jax.nn.silu(gate) * up_value).astype(jnp.bfloat16)
    terms = jnp.dot(hidden, down_full, preferred_element_type=jnp.float32)
    line_terms = lax.psum_scatter(
        terms.astype(jnp.bfloat16), "tp", scatter_dimension=0, tiled=True
    )
    ffn = lax.psum_scatter(
        line_terms, "sp", scatter_dimension=0, tiled=True, axis_index_groups=lines
    ).astype(jnp.float32)
    ffn = swap_blocks(ffn, blocks, ways)
    finished = (mid.astype(jnp.float32) + ffn).astype(jnp.bfloat16)
    return lax.all_gather(finished, "tp", axis=0, tiled=True)


def solution(mesh):
    in_specs = (
        P("sp", "tp"),
        P("sp", "tp"),
        P("sp", "tp"),
        P("tp", None),
        P("tp", None),
        P("tp", None),
        P("sp", None),
        P(),
        P("sp", "tp"),
        P("sp", "tp"),
        P("tp", "sp"),
    )
    out_specs = P("sp", None)
    return jax.shard_map(body, mesh=mesh, in_specs=in_specs, out_specs=out_specs, check_vma=False)
```
